32 devices in a mesh: rep: 2 (over x), fs: 8 (over z, y), tp: 2 (over core).
Axes of the slice: x: 2, y: 2, z: 4, core: 2. Of those that a mesh axis runs over, the one named last changes fastest.
Arguments:
- tokens: bfloat16 [8192, 2048], P(('rep', 'fs')), may hold values from -3 to 3
- mixer_gain: float32 [2048], replicated, may hold values from 0.1 to 1.9
- mix_weight: bfloat16 [2048, 1024], P('fs', 'tp'), may hold values from -0.125 to 0.125
- mixer_conv: float32 [4, 1024], P(None, 'tp'), may hold values from -3 to 3
- mixer_offset: float32 [1024], P('tp'), may hold values from -0.06 to 0.06
- recur_weight: bfloat16 [8, 128, 128], P('tp'), may hold values from -0.5 to 0.5
- recur_bias: float32 [1024], P('tp'), may hold values from -3 to 3
- input_weight: bfloat16 [8, 128, 128], P('tp'), may hold values from -0.5 to 0.5
- input_bias: float32 [1024], P('tp'), may hold values from 1 to 3
- decay_logit: float32 [1024], P('tp'), may hold values from 4 to 11
- out_weight: bfloat16 [1024, 2048], P('tp', 'fs'), may hold values from -0.375 to 0.375
- channel_gain: float32 [2048], replicated, may hold values from 0.1 to 1.9
- gate_weight: bfloat16 [2048, 6144], P('fs', 'tp'), may hold values from -0.125 to 0.125
- up_weight: bfloat16 [2048, 6144], P('fs', 'tp'), may hold values from -0.125 to 0.125
- gate_conv: float32 [3, 6144], P(None, 'tp'), may hold values from -3.5 to 3.5
- gate_offset: float32 [6144], P('tp'), may hold values from -3 to 3
- down_weight: bfloat16 [6144, 2048], P('tp', 'fs'), may hold values from -0.078125 to 0.078125
Outputs:
- layer_out: bfloat16 [8192, 2048], P(('rep', 'fs'))
The draws below stay inside these ranges and needn't reach their ends.
All inputs are finite; a program needn't handle non-finite values.
Results may differ from the reference program's by a relative error of at most 0.023.
Values may be sent and summed in bfloat16 or wider, within the bound.
No kernel may reach another device: no remote copies, remote signals or barrier semaphores. Data moves between devices by JAX's collectives and lax.ppermute only.
A program may use at most 128 MiB of HBM per device.

```python
import jax
import jax.numpy as jnp
from jax import lax

D = 2048
LRU = 1024
BLOCKS = 8
BLOCK_DIM = 128
MIX_TAPS = 4
FF = 6144
MLP_TAPS = 3
SEQLEN = 512
SEQS = 16
TOKENS = 8192
N_TP = 2


def draw_decay_logit(key, part):
    pick_key = jax.random.fold_in(key, 11)
    slow_key = jax.random.fold_in(key, 12)
    fast_key = jax.random.fold_in(key, 13)
    fast_share = 0.5
    fast = jax.random.bernoulli(pick_key, fast_share, (LRU,))
    slow_rate = jax.random.uniform(slow_key, (LRU,), jnp.float32, 1.0, 2.3) / SEQLEN
    fast_rate = jax.random.uniform(fast_key, (LRU,), jnp.float32, 0.02, 0.08)
    rate = jnp.where(fast, fast_rate, slow_rate) / 8.0
    return -rate - jnp.log(-jnp.expm1(-rate))


def steps_of(rng, shape, pieces, least, top_value):
    loudness, own = 1.0, jax.random.fold_in(rng, 6)
    for axis_at, blocks in pieces:
        draws = jnp.exp(jax.random.uniform(jax.random.fold_in(own, axis_at), (blocks,), jnp.float32, least / len(pieces), top_value / len(pieces)))
        loudness = loudness * jnp.repeat(draws, shape[axis_at] // blocks).reshape([-1 if axis == axis_at else 1 for axis in range(len(shape))])
    return loudness


def scatter_about(own_key, shape, spread, bound, cuts=(), kind=jnp.bfloat16):
    entries = spread * jax.random.normal(own_key, shape, jnp.float32)
    if cuts:
        entries = entries * steps_of(own_key, shape, cuts, -0.22, 0.18)
    return jnp.clip(entries, -bound, bound).astype(kind)


def setup_inputs(seed: int = 0) -> dict:
    keys = jax.random.split(jax.random.key(seed), 18)
    return {
        "tokens": scatter_about(keys[0], (TOKENS, D), 0.5, 3.0, ((0, 16),)),
        "mixer_gain": jnp.clip(1.0 + 0.18 * jax.random.normal(keys[1], (D,), jnp.float32), 0.1, 1.9),
        "mix_weight": scatter_about(keys[2], (D, LRU), D ** -0.5, 0.125, ((0, 8), (1, 2))),
        "mixer_conv": scatter_about(keys[3], (MIX_TAPS, LRU), MIX_TAPS ** -0.5, 3.0, ((1, 2),), jnp.float32),
        "mixer_offset": scatter_about(keys[4], (LRU,), 0.02, 0.06, ((0, 2),), jnp.float32),
        "recur_weight": scatter_about(keys[5], (BLOCKS, BLOCK_DIM, BLOCK_DIM), BLOCK_DIM ** -0.5, 0.5, ((0, 2),)),
        "recur_bias": scatter_about(keys[6], (LRU,), 0.5, 3.0, ((0, 2),), jnp.float32),
        "input_weight": scatter_about(keys[7], (BLOCKS, BLOCK_DIM, BLOCK_DIM), BLOCK_DIM ** -0.5, 0.5, ((0, 2),)),
        "input_bias": jnp.clip(1.0 + 2.0 * jax.random.uniform(keys[8], (LRU,), jnp.float32) ** steps_of(keys[8], (LRU,), ((0, 2),), -0.2, 0.2), 1.0, 3.0),
        "decay_logit": draw_decay_logit(jax.random.fold_in(keys[17], 71), 0),
        "out_weight": scatter_about(keys[10], (LRU, D), (LRU // 4) ** -0.5, 0.375, ((0, 2), (1, 8))),
        "channel_gain": jnp.clip(1.0 + 0.18 * jax.random.normal(keys[11], (D,), jnp.float32), 0.1, 1.9),
        "gate_weight": scatter_about(keys[12], (D, FF), D ** -0.5, 0.125, ((0, 8), (1, 2))),
        "up_weight": scatter_about(keys[13], (D, FF), D ** -0.5, 0.125, ((0, 8), (1, 2))),
        "gate_conv": scatter_about(keys[14], (MLP_TAPS, FF), MLP_TAPS ** -0.5, 3.5, ((1, 2),), jnp.float32),
        "gate_offset": scatter_about(keys[15], (FF,), 0.5, 3.0, ((0, 2),), jnp.float32),
        "down_weight": scatter_about(keys[16], (FF, D), FF ** -0.5, 0.078125, ((0, 2), (1, 8))),
    }


epsilon = 1e-06
lru_scale = 8.0

def rms_rows(values, gain_row):
    widened = values.astype(jnp.float32)
    scaled = widened * lax.rsqrt(lax.optimization_barrier(jnp.mean(widened * widened, axis=-1, keepdims=True)) + epsilon)
    return (scaled * gain_row).astype(jnp.bfloat16)

def causal_conv(values, tap_rows, offset):
    width = tap_rows.shape[0]
    length = values.shape[-2]
    padding = [(0, 0)] * (values.ndim - 2) + [(width - 1, 0), (0, 0)]
    padded = jnp.pad(values, padding)
    total = offset + padded[..., 0:length, :] * tap_rows[0]
    for tap_index in range(1, width):
        total = total + padded[..., tap_index:tap_index + length, :] * tap_rows[tap_index]
    return total

def linear_combine(earlier, latter):
    decay_early, sum_early = earlier
    decay_late, sum_late = latter
    return (decay_early * decay_late, decay_late * sum_early + sum_late)

def lru_recur(recur_gate, input_gate, smoothed, decay_logit, axis):
    log_decay = lru_scale * recur_gate * jax.nn.log_sigmoid(decay_logit)
    drive = jnp.sqrt(-jnp.expm1(2.0 * log_decay)) * (input_gate * smoothed.astype(jnp.float32))
    _, states = lax.associative_scan(linear_combine, (jnp.exp(log_decay), drive), axis=axis)
    return states.astype(jnp.bfloat16)

def group_sums(left, right, groups):
    width = left.shape[1] // groups

    def add_group(total, index):
        left_part = lax.dynamic_slice_in_dim(left, index * width, width, 1)
        right_part = lax.dynamic_slice_in_dim(right, index * width, width, 0)
        partial_sum = jnp.dot(left_part, right_part, preferred_element_type=jnp.float32)
        rounded = lax.optimization_barrier(partial_sum.astype(jnp.bfloat16))
        return (total + rounded.astype(jnp.float32), None)
    start_total = jnp.zeros((left.shape[0], right.shape[1]), jnp.float32)
    total, _ = lax.scan(add_group, start_total, jnp.arange(groups, dtype=jnp.int32))
    return total

def block_gate(blocked, weight, bias):
    product = jnp.einsum('slhi,hij->slhj', blocked, weight.astype(jnp.float32))
    return jax.nn.sigmoid(product.reshape(SEQS, SEQLEN, LRU) + bias)

def reference(tokens, mixer_gain, mix_weight, mixer_conv, mixer_offset, recur_weight, recur_bias, input_weight, input_bias, decay_logit, out_weight, channel_gain, gate_weight, up_weight, gate_conv, gate_offset, down_weight):
    normed = rms_rows(tokens, mixer_gain)
    branch = jnp.dot(normed, mix_weight, preferred_element_type=jnp.float32).astype(jnp.bfloat16)
    branch = branch.reshape(SEQS, SEQLEN, LRU)
    smoothed = causal_conv(branch.astype(jnp.float32), mixer_conv, mixer_offset).astype(jnp.bfloat16)
    blocked = smoothed.reshape(SEQS, SEQLEN, BLOCKS, BLOCK_DIM).astype(jnp.float32)
    recur_gate = block_gate(blocked, recur_weight, recur_bias)
    input_gate = block_gate(blocked, input_weight, input_bias)
    recurrent = lru_recur(recur_gate, input_gate, smoothed, decay_logit, 1).reshape(TOKENS, LRU)
    mixer_sum = group_sums(recurrent, out_weight, N_TP)
    residual = (tokens.astype(jnp.float32) + mixer_sum).astype(jnp.bfloat16)
    normed_mlp = rms_rows(residual, channel_gain)
    gate_rows = jnp.dot(normed_mlp, gate_weight, preferred_element_type=jnp.float32).astype(jnp.bfloat16)
    up_rows = jnp.dot(normed_mlp, up_weight, preferred_element_type=jnp.float32).astype(jnp.bfloat16)
    gate_mixed = causal_conv(gate_rows.reshape(SEQS, SEQLEN, FF).astype(jnp.float32), gate_conv, gate_offset)
    hidden = jax.nn.gelu(gate_mixed) * up_rows.reshape(SEQS, SEQLEN, FF).astype(jnp.float32)
    hidden = hidden.astype(jnp.bfloat16).reshape(TOKENS, FF)
    mlp_sum = group_sums(hidden, down_weight, N_TP)
    return (residual.astype(jnp.float32) + mlp_sum).astype(jnp.bfloat16)
```

```python
import jax
import jax.numpy as jnp
from jax import lax
from jax.experimental import pallas as pl
from jax.experimental.pallas import tpu as pltpu
from jax.sharding import Mesh
from jax.sharding import PartitionSpec as P

epsilon = 1e-06
lru_scale = 8.0
bf16 = jnp.bfloat16
f32 = jnp.float32


def rms(values, axes):
    return values * lax.rsqrt(jnp.mean(values * values, axis=axes, keepdims=True) + epsilon)


def shift(values, axis, size, step):
    return lax.ppermute(values, axis, [(i, (i + step) % size) for i in range(size)])


def spread(values, axis, size):
    return [values] + [shift(values, axis, size, step) for step in range(1, size)]


def dot(left, right):
    return jnp.dot(left, right, preferred_element_type=f32)


def vmem(count):
    return [pl.BlockSpec(memory_space=pltpu.VMEM)] * count


smem = pl.BlockSpec(memory_space=pltpu.SMEM)


def delayed(values, rows, row):
    return jnp.where(row >= rows, pltpu.roll(values, rows, 0), 0.0)


def mixer_kernel(
    order,
    x,
    weight,
    taps,
    offset,
    recur_weight,
    recur_bias,
    input_weight,
    input_bias,
    rate,
    out,
    decay_ref,
    sum_ref,
):
    pieces = weight.shape[0]
    total = dot(x[order[0]], weight[0])
    for k in range(1, pieces):
        total = total + dot(x[order[k]], weight[k])
    branch = total.astype(bf16).astype(f32)
    length, width = branch.shape
    row = lax.broadcasted_iota(jnp.int32, branch.shape, 0)
    count = taps.shape[0]
    smoothed = offset[...] + branch * taps[count - 1 : count, :]
    for back in range(1, count):
        smoothed = smoothed + delayed(branch, back, row) * taps[count - 1 - back : count - back, :]
    smoothed = smoothed.astype(bf16)
    block = recur_weight.shape[1]
    recur = []
    inputs = []
    for k in range(recur_weight.shape[0]):
        part = smoothed[:, k * block : (k + 1) * block]
        recur.append(dot(part, recur_weight[k]))
        inputs.append(dot(part, input_weight[k]))
    recur_gate = jax.nn.sigmoid(jnp.concatenate(recur, axis=1) + recur_bias[...])
    input_gate = jax.nn.sigmoid(jnp.concatenate(inputs, axis=1) + input_bias[...])
    log_decay = recur_gate * rate[...]
    decay = jnp.exp(log_decay)
    gain = jnp.sqrt(-jnp.tanh(log_decay) * (1.0 + decay * decay))
    state = gain * (input_gate * smoothed.astype(f32))
    inner = row % 8
    for step in (1, 2, 4):
        keep = inner >= step
        before = jnp.where(keep, pltpu.roll(state, step, 0), 0.0)
        state = decay * before + state
        decay = decay * jnp.where(keep, pltpu.roll(decay, step, 0), 1.0)
    decay_ref[...] = decay
    sum_ref[...] = state

    def advance(tile, carry):
        at = pl.ds(pl.multiple_of(tile * 8, 8), 8)
        here = decay_ref[at, :] * carry + sum_ref[at, :]
        sum_ref[at, :] = here
        return jnp.broadcast_to(here[7:8, :], here.shape)

    lax.fori_loop(0, length // 8, advance, jnp.zeros((8, width), f32), unroll=4)
    share = out.shape[2]
    for k in range(out.shape[0]):
        out[k] = sum_ref[:, k * share : (k + 1) * share].astype(bf16)


def mixer(order, x, weight, taps, offset, recur_weight, recur_bias, input_weight, input_bias, rate):
    pieces, length, _ = x.shape
    channels = weight.shape[-1]
    blocks, block = recur_weight.shape[:2]
    steps = 1 if blocks % 2 else 2
    width = channels // steps
    count = blocks // steps
    whole = lambda a: pl.BlockSpec(a.shape, lambda i: (0,) * a.ndim)
    vec = lambda n: pl.BlockSpec((n, width), lambda i: (0, i))
    maps = pl.BlockSpec((count, block, block), lambda i: (i, 0, 0))
    return pl.pallas_call(
        mixer_kernel,
        grid=(steps,),
        in_specs=[
            smem,
            whole(x),
            pl.BlockSpec((pieces, weight.shape[1], width), lambda i: (0, 0, i)),
            vec(taps.shape[0]),
            vec(1),
            maps,
            vec(1),
            maps,
            vec(1),
            vec(1),
        ],
        out_specs=pl.BlockSpec((2 // steps, length, channels // 2), lambda i: (i, 0, 0)),
        out_shape=jax.ShapeDtypeStruct((2, length, channels // 2), bf16),
        scratch_shapes=[pltpu.VMEM((length, width), f32)] * 2,
        compiler_params=pltpu.CompilerParams(vmem_limit_bytes=48 << 20),
    )(order, x, weight, taps, offset, recur_weight, recur_bias, input_weight, input_bias, rate)


def project_kernel(order, first, recurrent, weight, *outs):
    rows = outs[0].shape[1]
    for part, out in enumerate(outs):
        at = pl.ds(pl.multiple_of(first[1 + part], rows), rows)
        left = [recurrent[first[0], at, :], recurrent[1 - first[0], at, :]]
        for k in range(weight.shape[1]):
            total = dot(left[0], weight[0, k]) + dot(left[1], weight[1, k])
            out[order[k]] = total.astype(bf16)


def project(order, first, recurrent, weight, parts):
    pieces, _, columns = weight.shape[1:]
    rows = recurrent.shape[1] // parts
    return pl.pallas_call(
        project_kernel,
        in_specs=[smem, smem] + vmem(2),
        out_specs=vmem(parts),
        out_shape=[jax.ShapeDtypeStruct((pieces, rows, columns), bf16)] * parts,
        compiler_params=pltpu.CompilerParams(vmem_limit_bytes=48 << 20),
    )(order, first, recurrent, weight)


def hidden_kernel(order, starts, taps, offset, *refs):
    parts = starts.shape[0]
    xs, refs = refs[:parts], refs[parts:]
    out, gate_ref, up_ref = refs[-3:]
    stacks = refs[:-3]
    half = len(stacks) // 2
    rows = xs[0].shape[1]
    for part, x in enumerate(xs):
        gate = up = None
        at = 0
        for stack in range(half):
            for k in range(stacks[stack].shape[0]):
                left = x[order[at]]
                at += 1
                more_gate = dot(left, stacks[stack][k])
                more_up = dot(left, stacks[half + stack][k])
                gate = more_gate if gate is None else gate + more_gate
                up = more_up if up is None else up + more_up
        where = pl.ds(pl.multiple_of(starts[part], rows), rows)
        gate_ref[where, :] = gate.astype(bf16).astype(f32)
        up_ref[where, :] = up.astype(bf16)
    gate = gate_ref[...]
    row = lax.broadcasted_iota(jnp.int32, gate.shape, 0)
    count = taps.shape[0]
    mixed = offset[...] + gate * taps[count - 1 : count, :]
    for back in range(1, count):
        mixed = mixed + delayed(gate, back, row) * taps[count - 1 - back : count - back, :]
    out[...] = (jax.nn.gelu(mixed) * up_ref[...].astype(f32)).astype(bf16)


def hidden_rows(order, starts, taps, offset, xs, gates, ups):
    rows = sum(x.shape[1] for x in xs)
    units = taps.shape[1]
    return pl.pallas_call(
        hidden_kernel,
        in_specs=[smem, smem] + vmem(2 + len(xs) + len(gates) + len(ups)),
        out_specs=vmem(1)[0],
        out_shape=jax.ShapeDtypeStruct((rows, units), bf16),
        scratch_shapes=[pltpu.VMEM((rows, units), f32), pltpu.VMEM((rows, units), bf16)],
        compiler_params=pltpu.CompilerParams(vmem_limit_bytes=56 << 20),
    )(order, starts, taps, offset, *xs, *gates, *ups)


def down_kernel(order, starts, weight, *refs):
    parts = starts.shape[0]
    hiddens, outs = refs[:-parts], refs[-parts:]
    for part, out in enumerate(outs):
        rows = out.shape[2]
        at = pl.ds(pl.multiple_of(starts[part], rows), rows)
        for s, hidden in enumerate(hiddens):
            left = hidden[at, :]
            for k in range(weight.shape[0]):
                out[s, order[k]] = dot(left, weight[k]).astype(bf16)


def down_rows(order, starts, weight, hiddens, parts):
    rows = hiddens[0].shape[0] // parts
    shape = (len(hiddens), weight.shape[0], rows, weight.shape[2])
    return pl.pallas_call(
        down_kernel,
        in_specs=[smem, smem] + vmem(1 + len(hiddens)),
        out_specs=vmem(parts),
        out_shape=[jax.ShapeDtypeStruct(shape, bf16)] * parts,
        compiler_params=pltpu.CompilerParams(vmem_limit_bytes=48 << 20),
    )(order, starts, weight, *hiddens)


def layer(sizes):
    R, A, B, C, T = (sizes[n] for n in ("rep", "fa", "fb", "fc", "tp"))
    F = A * B * C

    def local(
        tokens,
        mixer_gain,
        mix_weight,
        mixer_conv,
        mixer_offset,
        recur_weight,
        recur_bias,
        input_weight,
        input_bias,
        decay_logit,
        out_weight,
        channel_gain,
        gate_weight,
        up_weight,
        gate_conv,
        gate_offset,
        down_weight,
    ):
        r, a, b, c, t = (lax.axis_index(n) for n in ("rep", "fa", "fb", "fc", "tp"))
        length, model = tokens.shape
        slab = model // F
        rows = length // T

        def fs_of(da, db, dc):
            return (((a - da) % A) * B + (b - db) % B) * C + (c - dc) % C

        starts = jnp.stack([((t + k) % T) * rows for k in range(T)]).astype(jnp.int32)
        back_starts = jnp.stack([((t - k) % T) * rows for k in range(T)]).astype(jnp.int32)

        def plane(shard):
            half = shard.shape[0] // R
            own = lax.dynamic_slice_in_dim(shard, r * half, half, 0)
            along = jnp.stack(spread(own, "fa", A))
            along = jnp.stack(spread(along, "fb", B))
            side = shift(along, "fc", C, 1)
            other = shift(along, "rep", R, 1)
            far = jnp.concatenate(
                [shift(other[:1], "fc", C, 1), shift(side[1:], "rep", R, 1)], axis=0
            )
            return jnp.stack([along, side, other, far]).reshape(
                (R, C * B * A) + own.shape
            )

        plane_order = [fs_of(da, db, dc) for dc in range(C) for db in range(B) for da in range(A)]
        mix_full = plane(mix_weight)
        out_full = plane(out_weight)
        mix_order = jnp.stack(
            [f * R + (r - dr) % R for dr in range(R) for f in plane_order]
        ).astype(jnp.int32)
        out_order = jnp.stack(plane_order).astype(jnp.int32)

        def pieces(shard, axis):
            units = shard.shape[axis] // (R * B)

            def take(place):
                return lax.dynamic_slice_in_dim(shard, (r * B + place) * units, units, axis)

            own = [take(b)]
            for step in range(1, B):
                own.append(shift(take((b + step) % B), "fb", B, step))
            own = jnp.stack(own)
            found = []
            for near in spread(own, "fa", A):
                found.extend(spread(near, "fc", C))
            return found

        stack_ids = [(da, dc) for da in range(A) for dc in range(C)]
        gate_stacks = pieces(gate_weight, 1)
        up_stacks = pieces(up_weight, 1)
        down_stacks = pieces(down_weight, 0)
        hidden_order = jnp.stack(
            [fs_of(da, db, dc) for da, dc in stack_ids for db in range(B)]
        ).astype(jnp.int32)
        down_order = jnp.stack([(b - db) % B for db in range(B)]).astype(jnp.int32)

        def own_units(values):
            units = values.shape[-1] // (R * B)
            return lax.dynamic_slice_in_dim(values, (r * B + b) * units, units, values.ndim - 1)

        gate_taps = own_units(gate_conv)
        gate_shift = own_units(gate_offset)[None]

        normed = (rms(tokens.astype(f32), -1) * mixer_gain).astype(bf16)
        normed = normed.reshape(length, F * R, slab // R).transpose(1, 0, 2)
        rate = lru_scale * jax.nn.log_sigmoid(decay_logit)
        recurrent = mixer(
            mix_order,
            normed,
            mix_full.reshape((F * R,) + mix_full.shape[2:]),
            mixer_conv,
            mixer_offset[None],
            recur_weight,
            recur_bias[None],
            input_weight,
            input_bias[None],
            rate[None],
        )
        first = jnp.concatenate([r[None].astype(jnp.int32), starts])
        partials = project(out_order, first, recurrent, out_full, T)
        own_tokens = lax.dynamic_slice_in_dim(tokens, t * rows, rows, 0)
        own_tokens = own_tokens.reshape(rows, F, slab).transpose(1, 0, 2)
        total = partials[0].astype(f32)
        for step in range(1, T):
            total = total + shift(partials[step], "tp", T, step).astype(f32)
        residual = (own_tokens.astype(f32) + total).astype(bf16)
        gain = channel_gain.reshape(F, 1, slab)
        own_normed = (rms(residual.astype(f32), (0, 2)) * gain).astype(bf16)

        over_rep = shift(own_normed, "rep", R, 1)
        over_fb = shift(own_normed, "fb", B, 1)
        cut = F // 2
        over_both = jnp.concatenate(
            [shift(over_rep[:cut], "fb", B, 1), shift(over_fb[cut:], "rep", R, 1)], axis=0
        )
        hiddens = []
        for normed_rows in (own_normed, over_rep, over_fb, over_both):
            xs = spread(normed_rows, "tp", T)
            hiddens.append(
                hidden_rows(
                    hidden_order, back_starts, gate_taps, gate_shift, xs, gate_stacks, up_stacks
                )
            )

        columns = {}
        for place, (da, dc) in enumerate(stack_ids):
            parts = down_rows(down_order, starts, down_stacks[place], hiddens, T)
            total = parts[0].astype(f32)
            for step in range(1, T):
                total = total + shift(parts[step], "tp", T, step).astype(f32)
            if place % 2:
                axis, size, other, other_size = "fb", B, "rep", R
                sent, kept = (2, 3), (0, 1)
            else:
                axis, size, other, other_size = "rep", R, "fb", B
                sent, kept = (1, 3), (0, 2)
            rounded = total.astype(bf16)
            sent = jnp.stack([rounded[i] for i in sent])
            got = shift(sent, axis, size, 1).astype(f32)
            near = total[kept[0]] + got[0]
            far = (total[kept[1]] + got[1]).astype(bf16)
            columns[da, dc] = near + shift(far, other, other_size, 1).astype(f32)

        mlp_sum = jnp.stack(
            [columns[da, dc] for da, dc in stack_ids]
        )
        mlp_sum = mlp_sum.reshape((A, C, B) + mlp_sum.shape[2:])
        mlp_sum = jnp.take(mlp_sum, (a - jnp.arange(A)) % A, axis=0)
        mlp_sum = jnp.take(mlp_sum, (c - jnp.arange(C)) % C, axis=1)
        mlp_sum = mlp_sum.transpose(0, 2, 1, 3, 4).reshape(residual.shape)
        result = (residual.astype(f32) + mlp_sum).astype(bf16)
        result = result.transpose(1, 0, 2).reshape(rows, model)
        final = jnp.stack(spread(result, "tp", T))
        final = jnp.take(final, (t - jnp.arange(T)) % T, axis=0)
        return final.reshape(length, model)

    return local


def solution(mesh):
    shape = mesh.shape
    R, F, T = shape["rep"], shape["fs"], shape["tp"]
    sizes = {"rep": R, "fa": F // 4, "fb": 2, "fc": 2, "tp": T}
    devices = mesh.devices.reshape(tuple(sizes.values()))
    inner = Mesh(devices, tuple(sizes))
    fs = ("fa", "fb", "fc")
    in_specs = (
        P(("rep",) + fs, None),
        P(),
        P(fs, "tp"),
        P(None, "tp"),
        P("tp"),
        P("tp", None, None),
        P("tp"),
        P("tp", None, None),
        P("tp"),
        P("tp"),
        P("tp", fs),
        P(),
        P(fs, "tp"),
        P(fs, "tp"),
        P(None, "tp"),
        P("tp"),
        P("tp", fs),
    )
    out_specs = P(("rep",) + fs, None)
    return jax.shard_map(
        layer(sizes), mesh=inner, in_specs=in_specs, out_specs=out_specs, check_vma=False
    )
```
